32 devices in a mesh: grp: 2 (over y), sp: 4 (over z), tp: 4 (over x, core).
Axes of the slice: x: 2, y: 2, z: 4, core: 2. Of those that a mesh axis runs over, the one named last changes fastest.
Arguments:
- recurrent_query: bfloat16 [2048, 1024], P(('grp', 'sp'), 'tp'), parts along dimension 0, may hold values from -6 to 6
- recurrent_forget_gate: bfloat16 [2048, 1024], P(('grp', 'sp'), 'tp'), parts along dimension 0, may hold values from -4.5 to 4.5
- recurrent_value: bfloat16 [2048, 1024], P(('grp', 'sp'), 'tp'), parts along dimension 0, may hold values from -6 to 6
- recurrent_gate_lower_bound: float32 [1024], P('tp'), may hold values from 1.5 to 14
- recurrent_added_decay: float32 [2048, 8], P(('grp', 'sp'), 'tp'), parts along dimension 0, may hold values from -0.51 to 0
- recurrent_norm_gain: float32 [128], replicated, may hold values from 0.1 to 1.9
- attention_query_first: bfloat16 [2048, 512], P(('grp', 'sp'), 'tp'), parts along dimension 0, may hold values from -20 to 20
- attention_key_first: bfloat16 [2048, 256], P(('grp', 'sp'), 'tp'), parts along dimension 0, may hold values from -20 to 20
- attention_query_second: bfloat16 [2048, 512], P(('grp', 'sp'), 'tp'), parts along dimension 0, may hold values from -20 to 20
- attention_key_second: bfloat16 [2048, 256], P(('grp', 'sp'), 'tp'), parts along dimension 0, may hold values from -20 to 20
- attention_value: bfloat16 [2048, 512], P(('grp', 'sp'), 'tp'), parts along dimension 0, may hold values from -6 to 6
- second_map_weight: float32 [8], P('tp'), may hold values from 0.3 to 0.8
- attention_norm_gain: float32 [128], replicated, may hold values from 0.1 to 1.9
- output_weight: bfloat16 [2, 1024, 2048], P(None, 'tp', 'sp'), may hold values from -0.125 to 0.125
Outputs:
- mixed: bfloat16 [2048, 2048], P(('grp', 'sp', 'tp')), parts along dimension 0
The draws below stay inside these ranges and needn't reach their ends.
There are 2 independent parts, one for each index of `grp`. The reference program is written for one: setup_inputs(seed, part) draws one part's arguments, and reference() takes and returns one part's arrays. A program takes and returns all parts, laid end to end along the dimension named above; an argument that names none is the same for every part. Nothing has to cross between parts.
All inputs are finite; a program needn't handle non-finite values.
Results may differ from the reference program's by a relative error of at most 0.02.
Values may be sent and summed in bfloat16 or wider, within the bound.
A program may use at most 64 MiB of HBM per device.

```python
import jax
import jax.numpy as jnp
from jax import lax

D = 2048
RECURRENT_HEADS = 8
HG_DK = 128
HG_DV = 128
DA_HEADS = 8
KV_HEADS = 4
DA_HD = 64
BLK = 32
TOK_DEV = 256
TOKENS = 1024
MIX_WIDTH = 1024
N_TP = 4


def loguniform_draw(key, shape, low, high):
    return jnp.exp(jax.random.uniform(key, shape, jnp.float32, jnp.log(low), jnp.log(high)))


def draw_recurrent_gate_lower_bound(key, part):
    split_keys = jax.random.split(key, 4)
    order = jax.random.permutation(split_keys[0], RECURRENT_HEADS)
    fast = order < RECURRENT_HEADS // 2
    fast_rate = loguniform_draw(split_keys[1], (RECURRENT_HEADS,), 0.04, 0.12)
    slow_rate = loguniform_draw(split_keys[2], (RECURRENT_HEADS,), 0.3, 1.2) / TOKENS
    jitter = loguniform_draw(split_keys[3], (RECURRENT_HEADS, HG_DK), 0.7, 1.4)
    floor_rate = jnp.where(fast, fast_rate, slow_rate)[:, None] * jitter
    return jnp.log(1.0 / floor_rate - 1.0).reshape(-1).astype(jnp.float32)


def draw_recurrent_forget_gate(key, part):
    split_keys = jax.random.split(key, 2)
    block_count = TOKENS // TOK_DEV
    shift = jax.random.uniform(split_keys[0], (block_count, 1, RECURRENT_HEADS, 1), jnp.float32, -1.5, 1.5)
    rough = jax.random.truncated_normal(split_keys[1], -3.0, 3.0, (block_count, TOK_DEV, RECURRENT_HEADS, HG_DK), jnp.float32)
    return (rough + shift).reshape(TOKENS, RECURRENT_HEADS * HG_DK).astype(jnp.bfloat16)


def draw_recurrent_added_decay(key, part):
    split_keys = jax.random.split(key, 2)
    spots = jax.random.randint(split_keys[0], (3, RECURRENT_HEADS), 0, TOKENS)
    depth = jax.random.uniform(split_keys[1], (3, RECURRENT_HEADS), jnp.float32, -0.51, -0.22)
    matches = jnp.arange(TOKENS)[:, None, None] == spots[None]
    return jnp.min(jnp.where(matches, depth[None], 0.0), axis=1).astype(jnp.float32)


def draw_pair(key, marker):
    base = jax.random.fold_in(key, marker)
    split_keys = jax.random.split(base, 2)
    queries = 1.3 * jax.random.truncated_normal(split_keys[0], -6.0, 6.0, (TOKENS, DA_HEADS * DA_HD), jnp.float32)
    key_rows = 1.3 * jax.random.truncated_normal(split_keys[1], -6.0, 6.0, (TOKENS, KV_HEADS * DA_HD), jnp.float32)
    return (queries.astype(jnp.bfloat16), key_rows.astype(jnp.bfloat16))


def draw_attention_query_first(key, part):
    return draw_pair(key, 11)[0]


def draw_attention_key_first(key, part):
    return draw_pair(key, 11)[1]


def draw_attention_query_second(key, part):
    return draw_pair(key, 12)[0]


def draw_attention_key_second(key, part):
    return draw_pair(key, 12)[1]


def shard_levels(stream_key, shape, pieces, smallest, high):
    def one(axis_at, shards_of):
        draws = jax.random.uniform(jax.random.fold_in(jax.random.fold_in(stream_key, 6), axis_at), (shards_of,), jnp.float32, smallest / len(pieces), high / len(pieces))
        return jnp.repeat(jnp.exp(draws), shape[axis_at] // shards_of).reshape((-1,) + (1,) * (len(shape) - axis_at - 1))

    loudness = one(*pieces[0])
    for cut in pieces[1:]:
        loudness = loudness * one(*cut)
    return loudness


def scatter_about(rng, extent, width, most, cuts=(), held_as=jnp.bfloat16):
    loudness = shard_levels(rng, extent, cuts, -0.22, 0.18) if cuts else 1.0
    array = jax.random.normal(rng, extent, jnp.float32) * width * loudness
    return jnp.minimum(jnp.maximum(array, -most), most).astype(held_as)


def setup_inputs(seed: int = 0, part: int = 0) -> dict:
    keys = jax.random.split(jax.random.key(seed), 15)
    own_keys = jax.random.split(jax.random.fold_in(keys[14], part), 15)
    recurrent_query = scatter_about(own_keys[0], (TOKENS, RECURRENT_HEADS * HG_DK), 1.0, 6.0, ((0, 4), (1, 4)))
    recurrent_forget_gate = draw_recurrent_forget_gate(jax.random.fold_in(jax.random.fold_in(keys[14], part), 71), part)
    recurrent_value = scatter_about(own_keys[2], (TOKENS, MIX_WIDTH), 1.0, 6.0, ((0, 4), (1, 4)))
    recurrent_gate_lower_bound = draw_recurrent_gate_lower_bound(jax.random.fold_in(keys[14], 71), part)
    recurrent_added_decay = draw_recurrent_added_decay(jax.random.fold_in(jax.random.fold_in(keys[14], part), 71), part)
    recurrent_norm_gain = jnp.clip(1.0 + 0.18 * jax.random.normal(keys[5], (HG_DV,), jnp.float32), 0.1, 1.9)
    attention_query_first = draw_attention_query_first(jax.random.fold_in(jax.random.fold_in(keys[14], part), 71), part)
    attention_key_first = draw_attention_key_first(jax.random.fold_in(jax.random.fold_in(keys[14], part), 71), part)
    attention_query_second = draw_attention_query_second(jax.random.fold_in(jax.random.fold_in(keys[14], part), 71), part)
    attention_key_second = draw_attention_key_second(jax.random.fold_in(jax.random.fold_in(keys[14], part), 71), part)
    attention_value = scatter_about(own_keys[10], (TOKENS, KV_HEADS * 2 * DA_HD), 1.0, 6.0, ((0, 4), (1, 4)))
    second_map_weight = jnp.clip(0.3 + 0.5 * jax.random.uniform(keys[11], (DA_HEADS,), jnp.float32) ** shard_levels(keys[11], (DA_HEADS,), ((0, 4),), -0.2, 0.2), 0.3, 0.8)
    attention_norm_gain = jnp.clip(1.0 + 0.18 * jax.random.normal(keys[12], (2 * DA_HD,), jnp.float32), 0.1, 1.9)
    output_weight = scatter_about(keys[13], (2, MIX_WIDTH, D), (2 * MIX_WIDTH) ** -0.5, 0.125, ((1, 4), (2, 4)))
    return dict(recurrent_query=recurrent_query, recurrent_forget_gate=recurrent_forget_gate, recurrent_value=recurrent_value, recurrent_gate_lower_bound=recurrent_gate_lower_bound, recurrent_added_decay=recurrent_added_decay, recurrent_norm_gain=recurrent_norm_gain, attention_query_first=attention_query_first, attention_key_first=attention_key_first, attention_query_second=attention_query_second, attention_key_second=attention_key_second, attention_value=attention_value, second_map_weight=second_map_weight, attention_norm_gain=attention_norm_gain, output_weight=output_weight)


epsilon = 1e-06
highest = lax.Precision.HIGHEST

def head_norm(head_values, gain_vec):
    mean_square = lax.optimization_barrier(jnp.mean(head_values * head_values, axis=-1, keepdims=True))
    return head_values * lax.rsqrt(mean_square + epsilon) * gain_vec

def decay_factors(gate_preactivation, lower_bound_logit, added_log_decay, number_of_heads):
    token_count = gate_preactivation.shape[0]
    floor_rate = jax.nn.sigmoid(-lower_bound_logit).reshape(number_of_heads, -1)
    state_inflow = floor_rate[None] * jax.nn.sigmoid(-gate_preactivation.astype(jnp.float32)).reshape(token_count, number_of_heads, -1)
    decay_logarithm = jnp.log1p(-state_inflow) + added_log_decay[:, :, None]
    return (state_inflow, decay_logarithm)

def recurrence_blocks(queries, decay_logarithm, state_inflow, value_rows, block_len):
    token_count, number_of_heads, key_width = queries.shape
    block_count = token_count // block_len

    def to_blocks(source):
        return source.reshape(block_count, block_len, number_of_heads, source.shape[-1])
    causal = jnp.tril(jnp.ones((block_len, block_len), jnp.float32))[:, :, None, None]

    def block_step(carry_state, inputs):
        query_blk, decay_blk, inflow_blk, value_blk = inputs
        cumulative = jnp.cumsum(decay_blk, axis=0)
        relative = cumulative[:, None] - cumulative[None, :]
        decay_table = jnp.exp(jnp.minimum(relative, 0.0)) * causal
        scores = jnp.einsum('thd,shd,tshd->hts', query_blk, inflow_blk, decay_table, precision=highest)
        block_out = jnp.einsum('hts,shv->thv', scores, value_blk, precision=highest)
        block_out = block_out + jnp.einsum('thd,hdv->thv', query_blk * jnp.exp(cumulative), carry_state, precision=highest)
        last_log = cumulative[-1]
        new_state = jnp.exp(last_log)[:, :, None] * carry_state + jnp.einsum('shd,shv->hdv', inflow_blk * jnp.exp(last_log[None] - cumulative), value_blk, precision=highest)
        return (new_state, block_out)
    zero_state = jnp.zeros((number_of_heads, key_width, value_rows.shape[-1]), jnp.float32)
    final_state, outputs = lax.scan(block_step, zero_state, (to_blocks(queries), to_blocks(decay_logarithm), to_blocks(state_inflow), to_blocks(value_rows)))
    return (final_state, outputs.reshape(token_count, number_of_heads, -1))

def recurrent_token_mixer(recurrent_query, recurrent_forget_gate, recurrent_value, recurrent_gate_lower_bound, recurrent_added_decay, recurrent_norm_gain):
    token_count = recurrent_query.shape[0]
    state_inflow, decay_logarithm = decay_factors(recurrent_forget_gate, recurrent_gate_lower_bound, recurrent_added_decay, RECURRENT_HEADS)
    queries = recurrent_query.astype(jnp.float32).reshape(token_count, RECURRENT_HEADS, HG_DK)
    value_rows = recurrent_value.astype(jnp.float32).reshape(token_count, RECURRENT_HEADS, HG_DV)
    unused, mixed_rows = recurrence_blocks(queries, decay_logarithm, state_inflow, value_rows, BLK)
    return head_norm(mixed_rows, recurrent_norm_gain).astype(jnp.bfloat16)

def difference_mixer(attention_query_first, attention_key_first, attention_query_second, attention_key_second, attention_value, second_map_weight, attention_norm_gain):
    token_count = attention_query_first.shape[0]
    group_size = DA_HEADS // KV_HEADS
    score_scale = DA_HD ** (-0.5)
    keys_one = attention_key_first.astype(jnp.float32).reshape(token_count, KV_HEADS, DA_HD)
    keys_two = attention_key_second.astype(jnp.float32).reshape(token_count, KV_HEADS, DA_HD)
    value_rows = attention_value.astype(jnp.float32).reshape(token_count, KV_HEADS, 2 * DA_HD)
    lambda_table = second_map_weight.reshape(KV_HEADS, group_size)
    key_pos = jnp.arange(token_count).astype(jnp.int32)

    def per_block(block_index):
        first_row = (block_index * TOK_DEV).astype(jnp.int32)
        query_pos = first_row + jnp.arange(TOK_DEV).astype(jnp.int32)
        allowed = key_pos[None, :] <= query_pos[:, None]

        def slice_queries(source):
            picked = lax.dynamic_slice_in_dim(source, first_row, TOK_DEV, 0)
            return picked.astype(jnp.float32).reshape(TOK_DEV, KV_HEADS, group_size, DA_HD)
        queries_one = slice_queries(attention_query_first)
        queries_two = slice_queries(attention_query_second)

        def per_head(head_index):
            results = []
            for queries, key_rows in ((queries_one, keys_one), (queries_two, keys_two)):
                scores = jnp.einsum('qgd,sd->gqs', queries[:, head_index], key_rows[:, head_index], precision=highest) * score_scale
                scores = jnp.where(allowed[None], scores, -1e+30)
                row_max = lax.optimization_barrier(jnp.max(scores, axis=-1, keepdims=True))
                weights = jnp.where(allowed[None], jnp.exp(scores - row_max), 0.0)
                weight_mass = lax.optimization_barrier(jnp.sum(weights, axis=-1))
                rounded = lax.optimization_barrier(weights.astype(jnp.bfloat16)).astype(jnp.float32)
                product = jnp.einsum('gqs,sv->gqv', rounded, value_rows[:, head_index], precision=highest)
                results.append(product / weight_mass[..., None])
            return results[0] - lambda_table[head_index][:, None, None] * results[1]
        heads_out = lax.map(per_head, jnp.arange(KV_HEADS).astype(jnp.int32))
        return jnp.transpose(heads_out, (2, 0, 1, 3)).reshape(TOK_DEV, DA_HEADS, 2 * DA_HD)
    blocks = lax.map(per_block, jnp.arange(token_count // TOK_DEV).astype(jnp.int32))
    mixed_rows = blocks.reshape(token_count, DA_HEADS, 2 * DA_HD)
    return head_norm(mixed_rows, attention_norm_gain).astype(jnp.bfloat16)

def reference(recurrent_query, recurrent_forget_gate, recurrent_value, recurrent_gate_lower_bound, recurrent_added_decay, recurrent_norm_gain, attention_query_first, attention_key_first, attention_query_second, attention_key_second, attention_value, second_map_weight, attention_norm_gain, output_weight):
    recurrent_output = recurrent_token_mixer(recurrent_query, recurrent_forget_gate, recurrent_value, recurrent_gate_lower_bound, recurrent_added_decay, recurrent_norm_gain)
    attended = difference_mixer(attention_query_first, attention_key_first, attention_query_second, attention_key_second, attention_value, second_map_weight, attention_norm_gain)
    token_count = recurrent_query.shape[0]
    rec_share = RECURRENT_HEADS // N_TP
    att_share = DA_HEADS // N_TP
    row_share = MIX_WIDTH // N_TP
    summed = jnp.zeros((token_count, D), jnp.float32)
    for member in range(N_TP):
        rec_part = recurrent_output[:, member * rec_share:(member + 1) * rec_share].reshape(token_count, -1)
        att_part = attended[:, member * att_share:(member + 1) * att_share].reshape(token_count, -1)
        rows_rec = output_weight[0, member * row_share:(member + 1) * row_share]
        rows_att = output_weight[1, member * row_share:(member + 1) * row_share]
        partial_term = jnp.dot(rec_part, rows_rec, preferred_element_type=jnp.float32) + jnp.dot(att_part, rows_att, preferred_element_type=jnp.float32)
        summed = summed + lax.optimization_barrier(partial_term.astype(jnp.bfloat16)).astype(jnp.float32)
    return summed.astype(jnp.bfloat16)
```

```python
import jax
import jax.numpy as jnp
from jax import lax
from jax.experimental import pallas as pl
from jax.experimental.pallas import tpu as pltpu
from jax.sharding import PartitionSpec as P

HG_DK = 128
HG_DV = 128
DA_HD = 64
BLK = 32


epsilon = 1e-06
highest = lax.Precision.HIGHEST
key_span = 512


def carried_in(array, axis, combine, identity):
    size, place = (lax.axis_size(axis), lax.axis_index(axis))
    everything = jax.tree.map(
        lambda part, kind: lax.all_gather(part.astype(kind), axis),
        array,
        (jnp.bfloat16, jnp.bfloat16),
    )
    start = jax.tree.map(
        lambda part, zero: jnp.broadcast_to(jnp.asarray(zero, part.dtype), part.shape),
        array,
        identity,
    )

    def hop(k, before):
        reached = k < place
        new = combine(
            before, jax.tree.map(lambda part, own: part[k].astype(own.dtype), everything, array)
        )
        return jax.tree.map(lambda a, b: jnp.where(reached, a, b), new, before)

    return lax.fori_loop(0, size, hop, start)


def head_norm(head_values, gain_vec):
    mean_square = jnp.mean(head_values * head_values, axis=-1, keepdims=True)
    return head_values * lax.rsqrt(mean_square + epsilon) * gain_vec


def decay_factors(gate_preactivation, lower_bound_logit, added_log_decay, number_of_heads):
    token_count = gate_preactivation.shape[0]
    floor_rate = jax.nn.sigmoid(-lower_bound_logit).reshape(number_of_heads, -1)
    state_inflow = floor_rate[None] * jax.nn.sigmoid(
        -gate_preactivation.astype(jnp.float32)
    ).reshape(token_count, number_of_heads, -1)
    decay_logarithm = jnp.log1p(-state_inflow) + added_log_decay[:, :, None]
    return (state_inflow, decay_logarithm)


def recurrence_blocks(queries, decay_logarithm, state_inflow, value_rows, block_len):
    token_count, number_of_heads, key_width = queries.shape
    block_count = token_count // block_len

    def to_blocks(source):
        return source.reshape(block_count, block_len, number_of_heads, source.shape[-1])

    causal = jnp.tril(jnp.ones((block_len, block_len), jnp.float32))[:, :, None, None]

    def block_step(carry_state, inputs):
        query_blk, decay_blk, inflow_blk, value_blk = inputs
        cumulative = jnp.cumsum(decay_blk, axis=0)
        relative = cumulative[:, None] - cumulative[None, :]
        decay_table = jnp.exp(jnp.minimum(relative, 0.0)) * causal
        scores = jnp.einsum(
            "thd,shd,tshd->hts", query_blk, inflow_blk, decay_table, precision=highest
        )
        block_out = jnp.einsum("hts,shv->thv", scores, value_blk, precision=highest)
        block_out = block_out + jnp.einsum(
            "thd,hdv->thv", query_blk * jnp.exp(cumulative), carry_state, precision=highest
        )
        last_log = cumulative[-1]
        new_state = jnp.exp(last_log)[:, :, None] * carry_state + jnp.einsum(
            "shd,shv->hdv",
            inflow_blk * jnp.exp(last_log[None] - cumulative),
            value_blk,
            precision=highest,
        )
        return (new_state, block_out)

    zero_state = jnp.zeros((number_of_heads, key_width, value_rows.shape[-1]), jnp.float32)
    final_state, outputs = lax.scan(
        block_step,
        zero_state,
        (
            to_blocks(queries),
            to_blocks(decay_logarithm),
            to_blocks(state_inflow),
            to_blocks(value_rows),
        ),
    )
    return (final_state, outputs.reshape(token_count, number_of_heads, -1))


def chain_pair(earlier, following):
    return (earlier[0] * following[0], following[0][:, :, None] * earlier[1] + following[1])


def recurrent_path_output(
    recurrent_query,
    recurrent_forget_gate,
    recurrent_value,
    recurrent_gate_lower_bound,
    recurrent_added_decay,
    recurrent_norm_gain,
):
    token_count = recurrent_query.shape[0]
    number_of_heads = recurrent_gate_lower_bound.shape[0] // HG_DK
    state_inflow, decay_logarithm = decay_factors(
        recurrent_forget_gate, recurrent_gate_lower_bound, recurrent_added_decay, number_of_heads
    )
    queries = recurrent_query.astype(jnp.float32).reshape(token_count, number_of_heads, HG_DK)
    value_rows = recurrent_value.astype(jnp.float32).reshape(token_count, number_of_heads, HG_DV)
    final_state, local_out = recurrence_blocks(
        queries, decay_logarithm, state_inflow, value_rows, BLK
    )
    running_log = jnp.cumsum(decay_logarithm, axis=0)
    through = jnp.exp(running_log[-1])
    incoming = carried_in(
        (through, final_state),
        "sp",
        chain_pair,
        (jnp.ones_like(through), jnp.zeros_like(final_state)),
    )
    carried = jnp.einsum(
        "thd,hdv->thv", queries * jnp.exp(running_log), incoming[1], precision=highest
    )
    return (
        head_norm(local_out + carried, recurrent_norm_gain)
        .astype(jnp.bfloat16)
        .reshape(token_count, -1)
    )


def attention_branch(
    attention_query_first,
    attention_key_first,
    attention_query_second,
    attention_key_second,
    attention_value,
    second_map_weight,
    attention_norm_gain,
):
    query_rows = attention_query_first.shape[0]
    key_heads = attention_key_first.shape[1] // DA_HD
    group_size = attention_query_first.shape[1] // DA_HD // key_heads
    score_scale = DA_HD ** (-0.5)
    offset = lax.axis_index("sp") * query_rows
    query_pos = offset + jnp.arange(query_rows)
    last_query = offset + query_rows - 1
    queries_one = attention_query_first.reshape(query_rows, key_heads, group_size, DA_HD)
    queries_two = attention_query_second.reshape(query_rows, key_heads, group_size, DA_HD)

    def map_update(running, queries, key_rows, value_rows, allowed):
        row_max, weight_mass, value_sum = running
        scores = (
            jnp.einsum("qkgd,skd->kgqs", queries, key_rows, preferred_element_type=jnp.float32)
            * score_scale
        )
        scores = jnp.where(allowed, scores, -1e30)
        new_max = jnp.maximum(row_max, jnp.max(scores, axis=-1))
        weights = jnp.where(allowed, jnp.exp(scores - new_max[..., None]), 0.0)
        shrink = jnp.exp(row_max - new_max)
        weight_mass = weight_mass * shrink + jnp.sum(weights, axis=-1)
        value_sum = value_sum * shrink[..., None] + jnp.einsum(
            "plew,wpd->pled",
            weights.astype(jnp.bfloat16),
            value_rows,
            preferred_element_type=jnp.float32,
        )
        return (new_max, weight_mass, value_sum)

    def key_block(running, block_one, block_two, block_values, first_row):
        span_rows = block_one.shape[0]
        key_pos = first_row + jnp.arange(span_rows)
        allowed = key_pos[None, :] <= query_pos[:, None]
        shaped_one = block_one.reshape(span_rows, key_heads, DA_HD)
        shaped_two = block_two.reshape(span_rows, key_heads, DA_HD)
        shaped_values = block_values.reshape(span_rows, key_heads, 2 * DA_HD)
        return (
            map_update(running[0], queries_one, shaped_one, shaped_values, allowed),
            map_update(running[1], queries_two, shaped_two, shaped_values, allowed),
        )

    def guarded_block(running, block_one, block_two, block_values, first_row):

        def compute(state_in):
            return key_block(state_in, block_one, block_two, block_values, first_row)

        def unchanged(state_in):
            return state_in

        result = lax.cond(first_row > last_query, unchanged, compute, running)
        return result

    start_max = jnp.full((key_heads, group_size, query_rows), -1e30, jnp.float32)
    zero_mass = jnp.zeros((key_heads, group_size, query_rows), jnp.float32)
    zero_sum = jnp.zeros((key_heads, group_size, query_rows, 2 * DA_HD), jnp.float32)
    fresh_state = (start_max, zero_mass, zero_sum)
    running = (fresh_state, fresh_state)
    shard_one = lax.all_gather(attention_key_first, "sp", axis=0, tiled=True)
    shard_two = lax.all_gather(attention_key_second, "sp", axis=0, tiled=True)
    shard_values = lax.all_gather(attention_value, "sp", axis=0, tiled=True)
    row_count = shard_one.shape[0]
    span_rows = min(row_count, key_span)
    full_count = row_count // span_rows

    def span_step(span_index, state_in):
        begin_row = span_index * span_rows
        return guarded_block(
            state_in,
            lax.dynamic_slice_in_dim(shard_one, begin_row, span_rows, 0),
            lax.dynamic_slice_in_dim(shard_two, begin_row, span_rows, 0),
            lax.dynamic_slice_in_dim(shard_values, begin_row, span_rows, 0),
            begin_row,
        )

    running = lax.fori_loop(0, full_count, span_step, running)
    first_map, second_map = running
    lambda_table = second_map_weight.reshape(key_heads, group_size)[:, :, None, None]
    combined = first_map[2] / first_map[1][..., None] - lambda_table * (
        second_map[2] / second_map[1][..., None]
    )
    combined = jnp.transpose(combined, (2, 0, 1, 3)).reshape(
        query_rows, key_heads * group_size, 2 * DA_HD
    )
    return head_norm(combined, attention_norm_gain).astype(jnp.bfloat16).reshape(query_rows, -1)


def shards(
    recurrent_query,
    recurrent_forget_gate,
    recurrent_value,
    recurrent_gate_lower_bound,
    recurrent_added_decay,
    recurrent_norm_gain,
    attention_query_first,
    attention_key_first,
    attention_query_second,
    attention_key_second,
    attention_value,
    second_map_weight,
    attention_norm_gain,
    output_weight,
):
    attended = attention_branch(
        attention_query_first,
        attention_key_first,
        attention_query_second,
        attention_key_second,
        attention_value,
        second_map_weight,
        attention_norm_gain,
    )
    recurrent_output = recurrent_path_output(
        recurrent_query,
        recurrent_forget_gate,
        recurrent_value,
        recurrent_gate_lower_bound,
        recurrent_added_decay,
        recurrent_norm_gain,
    )
    pieces = lax.all_gather(output_weight, "sp", axis=2, tiled=True)
    partial_terms = jnp.dot(
        recurrent_output, pieces[0], preferred_element_type=jnp.float32
    ) + jnp.dot(attended, pieces[1], preferred_element_type=jnp.float32)
    return lax.psum_scatter(
        partial_terms.astype(jnp.bfloat16), "tp", scatter_dimension=0, tiled=True
    )


CHUNK = 64
MESH = pl.DeviceIdType.MESH
BF = jnp.bfloat16
F32 = jnp.float32


def nt(a, b):
    return lax.dot_general(a, b, (((1,), (1,)), ((), ())), preferred_element_type=F32)


def tn(a, b):
    return lax.dot_general(a, b, (((0,), (0,)), ((), ())), preferred_element_type=F32)


def nn(a, b):
    return jnp.dot(a, b, preferred_element_type=F32)


def layer_kernel(
    G, S, T,
    rq, fg, rv, lb, ad, rg, q1, k1, q2, k2, v, lam, ag, w,
    out,
    kv, wbuf, pbuf, rbuf, st_out, st_in, fst, rec, qrun, qs, m_ref, l_ref, acc, x,
    kv_send, kv_recv, st_send, st_recv, up_send, dn_send, wz_recv, wy_send, wy_recv,
    rs_send, rs_recv, loc,
):
    g, z, j = lax.axis_index("grp"), lax.axis_index("sp"), lax.axis_index("tp")
    rows = rq.shape[0]
    heads = rq.shape[1] // HG_DK
    groups = q1.shape[1] // DA_HD
    cols = w.shape[2]
    share = rows // T
    up, dn = z + 1, z - 1
    has_up, has_dn = z + 1 < S, z > 0

    own_w = pltpu.make_async_copy(w, wbuf.at[z], loc)
    own_w.start()

    lane = lax.broadcasted_iota(jnp.int32, (rows, 2 * DA_HD), 1)
    kv[z, 0] = jnp.concatenate([k1[...], k2[...]], axis=1)
    kv[z, 1] = v[...]

    barrier = pltpu.get_barrier_semaphore()

    @pl.when(has_up)
    def _():
        pl.semaphore_signal(barrier, inc=1, device_id={"sp": up}, device_id_type=MESH)

    @pl.when(has_dn)
    def _():
        pl.semaphore_signal(barrier, inc=1, device_id={"sp": dn}, device_id_type=MESH)

    if G == 2:
        pl.semaphore_signal(barrier, inc=1, device_id={"grp": 1 - g}, device_id_type=MESH)
    for o in range(1, T):
        pl.semaphore_signal(
            barrier, inc=1, device_id={"tp": lax.rem(j + o, T)}, device_id_type=MESH
        )
    pl.semaphore_wait(
        barrier, jnp.where(has_up, 1, 0) + jnp.where(has_dn, 1, 0) + (G - 1) + (T - 1)
    )

    def kv_copy(k, slot):
        return pltpu.make_async_remote_copy(
            src_ref=kv.at[k], dst_ref=kv.at[k], send_sem=kv_send.at[slot],
            recv_sem=kv_recv.at[k], device_id={"sp": up}, device_id_type=MESH)

    def half(ref):
        return ref.at[g] if G == 2 else ref

    def w_copy(k, slot, upward):
        source = half(w) if slot == 0 else half(wbuf.at[k])
        return pltpu.make_async_remote_copy(
            src_ref=source, dst_ref=half(wbuf.at[k]),
            send_sem=(up_send if upward else dn_send).at[slot], recv_sem=wz_recv.at[k],
            device_id={"sp": up if upward else dn}, device_id_type=MESH)

    def y_copy(k, which):
        return pltpu.make_async_remote_copy(
            src_ref=wbuf.at[k, which], dst_ref=wbuf.at[k, which],
            send_sem=wy_send.at[k], recv_sem=wy_recv.at[k],
            device_id={"grp": 1 - g}, device_id_type=MESH)

    def st_copy():
        return pltpu.make_async_remote_copy(
            src_ref=st_out, dst_ref=st_in, send_sem=st_send.at[0], recv_sem=st_recv.at[0],
            device_id={"sp": up}, device_id_type=MESH)

    def rs_copy(k, o):
        to = lax.rem(j + o, T)
        return pltpu.make_async_remote_copy(
            src_ref=pbuf.at[k, to], dst_ref=rbuf.at[o, k],
            send_sem=rs_send.at[k, o], recv_sem=rs_recv.at[k, o],
            device_id={"tp": to}, device_id_type=MESH)

    @pl.when(has_up)
    def _():
        kv_copy(z, 0).start()

    @pl.when(has_dn)
    def _():
        w_copy(z, 0, False).start()

    inflow = jax.nn.sigmoid(-lb[...]) * jax.nn.sigmoid(-fg[...].astype(F32))
    added = jnp.concatenate(
        [jnp.broadcast_to(ad[:, h : h + 1], (rows, HG_DK)) for h in range(heads)], axis=1
    )
    logd = jnp.log1p(-inflow) + added
    hi = logd.astype(BF)
    lo = (logd - hi.astype(F32)).astype(BF)
    ti = lax.broadcasted_iota(jnp.int32, (rows, rows), 0)
    si = lax.broadcasted_iota(jnp.int32, (rows, rows), 1)
    tril = ti >= si
    trib = jnp.where(tril, 1.0, 0.0).astype(BF)
    blockb = jnp.where(tril & (ti // CHUNK == si // CHUNK), 1.0, 0.0).astype(BF)
    cum = nn(blockb, hi) + nn(blockb, lo)
    run = nn(trib, hi) + nn(trib, lo)
    q = rq[...].astype(F32)
    qd = (q * jnp.exp(cum)).astype(BF)
    kd = (inflow * jnp.exp(-cum)).astype(BF)
    qrun[...] = (q * jnp.exp(run)).astype(BF)
    total = jnp.exp(run[rows - 1 : rows, :])
    small = (
        lax.broadcasted_iota(jnp.int32, (CHUNK, CHUNK), 0)
        >= lax.broadcasted_iota(jnp.int32, (CHUNK, CHUNK), 1)
    )
    for h in range(heads):
        cs = slice(h * HG_DK, (h + 1) * HG_DK)
        state = None
        for c in range(rows // CHUNK):
            rs = slice(c * CHUNK, (c + 1) * CHUNK)
            vc = rv[rs, cs]
            sc = jnp.where(small, nt(qd[rs, cs], kd[rs, cs]), 0.0).astype(BF)
            o = nn(sc, vc)
            if state is not None:
                o = o + nt(qd[rs, cs], state.astype(BF))
            rec[rs, cs] = o
            last = cum[(c + 1) * CHUNK - 1 : (c + 1) * CHUNK, cs]
            kend = (inflow[rs, cs] * jnp.exp(last - cum[rs, cs])).astype(BF)
            add = tn(vc, kend)
            state = add if state is None else jnp.exp(last) * state + add
        fst[h] = state

    @pl.when(jnp.logical_and(z == 0, has_up))
    def _():
        st_out[...] = fst[...].astype(BF)
        st_copy().start()

    def kv_arrive(d):
        @pl.when(z >= d)
        def _():
            kv_copy(z - d, 0).wait_recv()

            @pl.when(has_up)
            def _():
                kv_copy(z - d, d).start()

    q1f = q1[...].astype(F32) * (DA_HD ** -0.5)
    q2f = q2[...].astype(F32) * (DA_HD ** -0.5)
    low = lane < DA_HD
    for h in range(groups):
        a = jnp.concatenate([q1f[:, h * DA_HD : (h + 1) * DA_HD], jnp.zeros((rows, DA_HD), F32)], 1)
        b = jnp.concatenate([jnp.zeros((rows, DA_HD), F32), q2f[:, h * DA_HD : (h + 1) * DA_HD]], 1)
        qs[h] = a.astype(BF)
        qs[groups + h] = b.astype(BF)

    def attend(k, first):
        for r in range(2 * groups):
            s = nt(qs[r], kv[k, 0])
            if first:
                s = jnp.where(tril, s, -1e30)
                top = jnp.max(s, axis=1, keepdims=True)
            else:
                top = jnp.maximum(m_ref[r], jnp.max(s, axis=1, keepdims=True))
            p = jnp.exp(s - top)
            mass = jnp.sum(p, axis=1, keepdims=True)
            val = nn(p.astype(BF), kv[k, 1])
            if not first:
                shrink = jnp.exp(m_ref[r] - top)
                mass = mass + l_ref[r] * shrink
                val = val + acc[r] * shrink
            m_ref[r] = top
            l_ref[r] = mass
            acc[r] = val

    if S > 1:
        kv_arrive(1)
    attend(z, True)
    if S > 2:
        kv_arrive(2)

    @pl.when(has_dn)
    def _():
        st_copy().wait_recv()

        @pl.when(has_up)
        def _():
            for h in range(heads):
                st_out[h] = (
                    total[:, h * HG_DK : (h + 1) * HG_DK] * st_in[h].astype(F32) + fst[h]
                ).astype(BF)
            st_copy().start()

        for h in range(heads):
            cs = slice(h * HG_DK, (h + 1) * HG_DK)
            rec[:, cs] = rec[:, cs] + nt(qrun[:, cs], st_in[h])

    for d in range(3, S):
        kv_arrive(d)

    @pl.when(has_up)
    def _():
        w_copy(z, 0, True).start()

    def w_arrive(d, upward):
        k = z - d if upward else z + d
        there = (z >= d) if upward else (z + d < S)
        onward = has_up if upward else has_dn

        @pl.when(there)
        def _():
            w_copy(k, 1, upward).wait_recv()

            @pl.when(onward)
            def _():
                w_copy(k, d, upward).start()

            if G == 2:
                y_copy(k, g).start()

    w_arrive(1, False)
    for d in range(1, S):
        @pl.when(z >= d)
        def _(d=d):
            attend(z - d, False)

    for h in range(heads):
        cs = slice(h * HG_DK, (h + 1) * HG_DK)
        x[:, cs] = head_norm(rec[:, cs], rg[...]).astype(BF)
    for h in range(groups):
        mixed = acc[h] / l_ref[h] - lam[h] * (acc[groups + h] / l_ref[groups + h])
        base = heads * HG_DK + h * 2 * DA_HD
        x[:, base : base + 2 * DA_HD] = head_norm(mixed, ag[...]).astype(BF)

    split = heads * HG_DK

    def project(k):
        part = nn(x[:, :split], wbuf[k, 0]) + nn(x[:, split:], wbuf[k, 1])
        pbuf[k] = part.astype(BF).reshape(T, share, cols)
        for o in range(1, T):
            rs_copy(k, o).start()

    own_w.wait()
    project(z)

    def finish(d, upward):
        k = z - d if upward else z + d
        there = (z >= d) if upward else (z + d < S)

        @pl.when(there)
        def _():
            if G == 2:
                y_copy(k, 1 - g).wait_recv()
            project(k)

    for d in range(1, S):
        w_arrive(d, True)
        if d > 1:
            w_arrive(d, False)
            finish(d - 1, True)
            finish(d - 1, False)
    finish(S - 1, True)
    finish(S - 1, False)

    def gather_piece(k, carry):
        total_sum = pbuf[k, j].astype(F32)
        for o in range(1, T):
            rs_copy(k, o).wait_recv()
            total_sum = total_sum + rbuf[o, k].astype(F32)
        out[:, pl.ds(pl.multiple_of(k * cols, cols), cols)] = total_sum.astype(BF)
        return carry

    gather_piece(z, 0)
    for d in range(1, S):
        for upward in (True, False):
            @pl.when((z >= d) if upward else (z + d < S))
            def _(d=d, upward=upward):
                gather_piece(z - d if upward else z + d, 0)

    @pl.when(has_up)
    def _():
        st_copy().wait_send()

    for d in range(S):
        @pl.when(jnp.logical_and(z >= d, has_up))
        def _(d=d):
            kv_copy(z - d, d).wait_send()
            w_copy(z - d, d, True).wait_send()

        @pl.when(jnp.logical_and(z + d < S, has_dn))
        def _(d=d):
            w_copy(z + d, d, False).wait_send()

    if G == 2:
        for d in range(1, S):
            y_copy(lax.rem(z + d, S), g).wait_send()

    for k in range(S):
        for o in range(1, T):
            rs_copy(k, o).wait_send()


def fused_shards(G, S, T):
    def body(rq, fg, rv, lb, ad, rg, q1, k1, q2, k2, v, lam, ag, w):
        rows, cols = rq.shape[0], w.shape[2]
        heads, groups = rq.shape[1] // HG_DK, q1.shape[1] // DA_HD
        vm = pl.BlockSpec(memory_space=pltpu.VMEM)
        specs = [vm] * 14
        specs[11] = pl.BlockSpec(memory_space=pltpu.SMEM)
        specs[13] = pl.BlockSpec(memory_space=pl.ANY)
        dma = pltpu.SemaphoreType.DMA
        return pl.pallas_call(
            lambda *refs: layer_kernel(G, S, T, *refs),
            out_shape=jax.ShapeDtypeStruct((rows // T, cols * S), BF),
            in_specs=specs,
            out_specs=vm,
            scratch_shapes=[
                pltpu.VMEM((S, 2, rows, 2 * DA_HD), BF),
                pltpu.VMEM((S, 2, w.shape[1], cols), BF),
                pltpu.VMEM((S, T, rows // T, cols), BF),
                pltpu.VMEM((T, S, rows // T, cols), BF),
                pltpu.VMEM((heads, HG_DV, HG_DK), BF),
                pltpu.VMEM((heads, HG_DV, HG_DK), BF),
                pltpu.VMEM((heads, HG_DV, HG_DK), F32),
                pltpu.VMEM((rows, heads * HG_DV), F32),
                pltpu.VMEM((rows, heads * HG_DK), BF),
                pltpu.VMEM((2 * groups, rows, 2 * DA_HD), BF),
                pltpu.VMEM((2 * groups, rows, 1), F32),
                pltpu.VMEM((2 * groups, rows, 1), F32),
                pltpu.VMEM((2 * groups, rows, 2 * DA_HD), F32),
                pltpu.VMEM((rows, heads * HG_DV + groups * 2 * DA_HD), BF),
                dma((S,)), dma((S,)), dma((1,)), dma((1,)), dma((S,)), dma((S,)), dma((S,)),
                dma((S,)), dma((S,)), dma((S, T)), dma((S, T)), dma,
            ],
            compiler_params=pltpu.CompilerParams(collective_id=0, has_side_effects=True),
            name="layer",
        )(
            rq, fg, rv, lb.reshape(1, -1), ad, rg.reshape(1, -1),
            q1, k1, q2, k2, v, lam, ag.reshape(1, -1), w,
        )

    return body


def pick(G, S, T):
    def body(*args):
        rows, cols = args[0].shape[0], args[13].shape[2]
        one_key_head = args[7].shape[1] == DA_HD
        if cols % 128 or not one_key_head or S < 2 or G > 2 or rows % (T * 16) or S > 16:
            return shards(*args)
        return fused_shards(G, S, T)(*args)

    return body


def solution(mesh):
    return jax.shard_map(
        pick(mesh.shape["grp"], mesh.shape["sp"], mesh.shape["tp"]),
        mesh=mesh,
        in_specs=(
            P(("grp", "sp"), "tp"),
            P(("grp", "sp"), "tp"),
            P(("grp", "sp"), "tp"),
            P("tp"),
            P(("grp", "sp"), "tp"),
            P(),
            P(("grp", "sp"), "tp"),
            P(("grp", "sp"), "tp"),
            P(("grp", "sp"), "tp"),
            P(("grp", "sp"), "tp"),
            P(("grp", "sp"), "tp"),
            P("tp"),
            P(),
            P(None, "tp", "sp"),
        ),
        out_specs=P(("grp", "sp", "tp"), None),
        check_vma=False,
    )
```

```python
import jax
import jax.numpy as jnp
from jax import lax
from jax.experimental import pallas as pl
from jax.experimental.pallas import tpu as pltpu
from jax.sharding import PartitionSpec as P

HG_DK = 128
HG_DV = 128
DA_HD = 64
BLK = 32


epsilon = 1e-06
highest = lax.Precision.HIGHEST
key_span = 512


def carried_in(array, axis, combine, identity):
    size, place = (lax.axis_size(axis), lax.axis_index(axis))
    everything = jax.tree.map(
        lambda part, kind: lax.all_gather(part.astype(kind), axis),
        array,
        (jnp.bfloat16, jnp.bfloat16),
    )
    start = jax.tree.map(
        lambda part, zero: jnp.broadcast_to(jnp.asarray(zero, part.dtype), part.shape),
        array,
        identity,
    )

    def hop(k, before):
        reached = k < place
        new = combine(
            before, jax.tree.map(lambda part, own: part[k].astype(own.dtype), everything, array)
        )
        return jax.tree.map(lambda a, b: jnp.where(reached, a, b), new, before)

    return lax.fori_loop(0, size, hop, start)


def head_norm(head_values, gain_vec):
    mean_square = jnp.mean(head_values * head_values, axis=-1, keepdims=True)
    return head_values * lax.rsqrt(mean_square + epsilon) * gain_vec


def decay_factors(gate_preactivation, lower_bound_logit, added_log_decay, number_of_heads):
    token_count = gate_preactivation.shape[0]
    floor_rate = jax.nn.sigmoid(-lower_bound_logit).reshape(number_of_heads, -1)
    state_inflow = floor_rate[None] * jax.nn.sigmoid(
        -gate_preactivation.astype(jnp.float32)
    ).reshape(token_count, number_of_heads, -1)
    decay_logarithm = jnp.log1p(-state_inflow) + added_log_decay[:, :, None]
    return (state_inflow, decay_logarithm)


def recurrence_blocks(queries, decay_logarithm, state_inflow, value_rows, block_len):
    token_count, number_of_heads, key_width = queries.shape
    block_count = token_count // block_len

    def to_blocks(source):
        return source.reshape(block_count, block_len, number_of_heads, source.shape[-1])

    causal = jnp.tril(jnp.ones((block_len, block_len), jnp.float32))[:, :, None, None]

    def block_step(carry_state, inputs):
        query_blk, decay_blk, inflow_blk, value_blk = inputs
        cumulative = jnp.cumsum(decay_blk, axis=0)
        relative = cumulative[:, None] - cumulative[None, :]
        decay_table = jnp.exp(jnp.minimum(relative, 0.0)) * causal
        scores = jnp.einsum(
            "thd,shd,tshd->hts", query_blk, inflow_blk, decay_table, precision=highest
        )
        block_out = jnp.einsum("hts,shv->thv", scores, value_blk, precision=highest)
        block_out = block_out + jnp.einsum(
            "thd,hdv->thv", query_blk * jnp.exp(cumulative), carry_state, precision=highest
        )
        last_log = cumulative[-1]
        new_state = jnp.exp(last_log)[:, :, None] * carry_state + jnp.einsum(
            "shd,shv->hdv",
            inflow_blk * jnp.exp(last_log[None] - cumulative),
            value_blk,
            precision=highest,
        )
        return (new_state, block_out)

    zero_state = jnp.zeros((number_of_heads, key_width, value_rows.shape[-1]), jnp.float32)
    final_state, outputs = lax.scan(
        block_step,
        zero_state,
        (
            to_blocks(queries),
            to_blocks(decay_logarithm),
            to_blocks(state_inflow),
            to_blocks(value_rows),
        ),
    )
    return (final_state, outputs.reshape(token_count, number_of_heads, -1))


def chain_pair(earlier, following):
    return (earlier[0] * following[0], following[0][:, :, None] * earlier[1] + following[1])


def recurrent_path_output(
    recurrent_query,
    recurrent_forget_gate,
    recurrent_value,
    recurrent_gate_lower_bound,
    recurrent_added_decay,
    recurrent_norm_gain,
):
    token_count = recurrent_query.shape[0]
    number_of_heads = recurrent_gate_lower_bound.shape[0] // HG_DK
    state_inflow, decay_logarithm = decay_factors(
        recurrent_forget_gate, recurrent_gate_lower_bound, recurrent_added_decay, number_of_heads
    )
    queries = recurrent_query.astype(jnp.float32).reshape(token_count, number_of_heads, HG_DK)
    value_rows = recurrent_value.astype(jnp.float32).reshape(token_count, number_of_heads, HG_DV)
    final_state, local_out = recurrence_blocks(
        queries, decay_logarithm, state_inflow, value_rows, BLK
    )
    running_log = jnp.cumsum(decay_logarithm, axis=0)
    through = jnp.exp(running_log[-1])
    incoming = carried_in(
        (through, final_state),
        "sp",
        chain_pair,
        (jnp.ones_like(through), jnp.zeros_like(final_state)),
    )
    carried = jnp.einsum(
        "thd,hdv->thv", queries * jnp.exp(running_log), incoming[1], precision=highest
    )
    return (
        head_norm(local_out + carried, recurrent_norm_gain)
        .astype(jnp.bfloat16)
        .reshape(token_count, -1)
    )


def attention_branch(
    attention_query_first,
    attention_key_first,
    attention_query_second,
    attention_key_second,
    attention_value,
    second_map_weight,
    attention_norm_gain,
):
    query_rows = attention_query_first.shape[0]
    key_heads = attention_key_first.shape[1] // DA_HD
    group_size = attention_query_first.shape[1] // DA_HD // key_heads
    score_scale = DA_HD ** (-0.5)
    offset = lax.axis_index("sp") * query_rows
    query_pos = offset + jnp.arange(query_rows)
    last_query = offset + query_rows - 1
    queries_one = attention_query_first.reshape(query_rows, key_heads, group_size, DA_HD)
    queries_two = attention_query_second.reshape(query_rows, key_heads, group_size, DA_HD)

    def map_update(running, queries, key_rows, value_rows, allowed):
        row_max, weight_mass, value_sum = running
        scores = (
            jnp.einsum("qkgd,skd->kgqs", queries, key_rows, preferred_element_type=jnp.float32)
            * score_scale
        )
        scores = jnp.where(allowed, scores, -1e30)
        new_max = jnp.maximum(row_max, jnp.max(scores, axis=-1))
        weights = jnp.where(allowed, jnp.exp(scores - new_max[..., None]), 0.0)
        shrink = jnp.exp(row_max - new_max)
        weight_mass = weight_mass * shrink + jnp.sum(weights, axis=-1)
        value_sum = value_sum * shrink[..., None] + jnp.einsum(
            "plew,wpd->pled",
            weights.astype(jnp.bfloat16),
            value_rows,
            preferred_element_type=jnp.float32,
        )
        return (new_max, weight_mass, value_sum)

    def key_block(running, block_one, block_two, block_values, first_row):
        span_rows = block_one.shape[0]
        key_pos = first_row + jnp.arange(span_rows)
        allowed = key_pos[None, :] <= query_pos[:, None]
        shaped_one = block_one.reshape(span_rows, key_heads, DA_HD)
        shaped_two = block_two.reshape(span_rows, key_heads, DA_HD)
        shaped_values = block_values.reshape(span_rows, key_heads, 2 * DA_HD)
        return (
            map_update(running[0], queries_one, shaped_one, shaped_values, allowed),
            map_update(running[1], queries_two, shaped_two, shaped_values, allowed),
        )

    def guarded_block(running, block_one, block_two, block_values, first_row):

        def compute(state_in):
            return key_block(state_in, block_one, block_two, block_values, first_row)

        def unchanged(state_in):
            return state_in

        result = lax.cond(first_row > last_query, unchanged, compute, running)
        return result

    start_max = jnp.full((key_heads, group_size, query_rows), -1e30, jnp.float32)
    zero_mass = jnp.zeros((key_heads, group_size, query_rows), jnp.float32)
    zero_sum = jnp.zeros((key_heads, group_size, query_rows, 2 * DA_HD), jnp.float32)
    fresh_state = (start_max, zero_mass, zero_sum)
    running = (fresh_state, fresh_state)
    shard_one = lax.all_gather(attention_key_first, "sp", axis=0, tiled=True)
    shard_two = lax.all_gather(attention_key_second, "sp", axis=0, tiled=True)
    shard_values = lax.all_gather(attention_value, "sp", axis=0, tiled=True)
    row_count = shard_one.shape[0]
    span_rows = min(row_count, key_span)
    full_count = row_count // span_rows

    def span_step(span_index, state_in):
        begin_row = span_index * span_rows
        return guarded_block(
            state_in,
            lax.dynamic_slice_in_dim(shard_one, begin_row, span_rows, 0),
            lax.dynamic_slice_in_dim(shard_two, begin_row, span_rows, 0),
            lax.dynamic_slice_in_dim(shard_values, begin_row, span_rows, 0),
            begin_row,
        )

    running = lax.fori_loop(0, full_count, span_step, running)
    first_map, second_map = running
    lambda_table = second_map_weight.reshape(key_heads, group_size)[:, :, None, None]
    combined = first_map[2] / first_map[1][..., None] - lambda_table * (
        second_map[2] / second_map[1][..., None]
    )
    combined = jnp.transpose(combined, (2, 0, 1, 3)).reshape(
        query_rows, key_heads * group_size, 2 * DA_HD
    )
    return head_norm(combined, attention_norm_gain).astype(jnp.bfloat16).reshape(query_rows, -1)


def shards(
    recurrent_query,
    recurrent_forget_gate,
    recurrent_value,
    recurrent_gate_lower_bound,
    recurrent_added_decay,
    recurrent_norm_gain,
    attention_query_first,
    attention_key_first,
    attention_query_second,
    attention_key_second,
    attention_value,
    second_map_weight,
    attention_norm_gain,
    output_weight,
):
    attended = attention_branch(
        attention_query_first,
        attention_key_first,
        attention_query_second,
        attention_key_second,
        attention_value,
        second_map_weight,
        attention_norm_gain,
    )
    recurrent_output = recurrent_path_output(
        recurrent_query,
        recurrent_forget_gate,
        recurrent_value,
        recurrent_gate_lower_bound,
        recurrent_added_decay,
        recurrent_norm_gain,
    )
    pieces = lax.all_gather(output_weight, "sp", axis=2, tiled=True)
    partial_terms = jnp.dot(
        recurrent_output, pieces[0], preferred_element_type=jnp.float32
    ) + jnp.dot(attended, pieces[1], preferred_element_type=jnp.float32)
    return lax.psum_scatter(
        partial_terms.astype(jnp.bfloat16), "tp", scatter_dimension=0, tiled=True
    )


CHUNK = 64
PARTS = 2
MESH = pl.DeviceIdType.MESH
BF = jnp.bfloat16
F32 = jnp.float32


def nt(a, b):
    return lax.dot_general(a, b, (((1,), (1,)), ((), ())), preferred_element_type=F32)


def tn(a, b):
    return lax.dot_general(a, b, (((0,), (0,)), ((), ())), preferred_element_type=F32)


def nn(a, b):
    return jnp.dot(a, b, preferred_element_type=F32)


def layer_kernel(
    G, S, T,
    rq, fg, rv, lb, ad, rg, q1, k1, q2, k2, v, lam, ag, w,
    out,
    kt, vv, wbuf, pbuf, rbuf, st_out, st_in, fst, rec, qrun, qs, m_ref, l_ref, acc, x,
    kv_send, kv_recv, st_send, st_recv, up_send, dn_send, wz_recv, wy_send, wy_recv,
    rs_send, rs_recv, loc,
):
    g, z, j = lax.axis_index("grp"), lax.axis_index("sp"), lax.axis_index("tp")
    rows = rq.shape[0]
    heads = rq.shape[1] // HG_DK
    groups = q1.shape[1] // DA_HD
    cols = w.shape[2] // PARTS
    share = rows // T
    up, dn = z + 1, z - 1
    has_up, has_dn = z + 1 < S, z > 0

    own_w = [
        pltpu.make_async_copy(w.at[:, :, pl.ds(c * cols, cols)], wbuf.at[z, c], loc.at[c])
        for c in range(PARTS)
    ]
    for one in own_w:
        one.start()

    kt[z, :DA_HD] = k1[...]
    kt[z, DA_HD:] = k2[...]
    vv[z] = v[...]

    barrier = pltpu.get_barrier_semaphore()

    @pl.when(has_up)
    def _():
        pl.semaphore_signal(barrier, inc=1, device_id={"sp": up}, device_id_type=MESH)

    @pl.when(has_dn)
    def _():
        pl.semaphore_signal(barrier, inc=1, device_id={"sp": dn}, device_id_type=MESH)

    if G == 2:
        pl.semaphore_signal(barrier, inc=1, device_id={"grp": 1 - g}, device_id_type=MESH)
    for o in range(1, T):
        pl.semaphore_signal(
            barrier, inc=1, device_id={"tp": lax.rem(j + o, T)}, device_id_type=MESH
        )
    pl.semaphore_wait(
        barrier, jnp.where(has_up, 1, 0) + jnp.where(has_dn, 1, 0) + (G - 1) + (T - 1)
    )

    def kv_copies(k, slot):
        return [
            pltpu.make_async_remote_copy(
                src_ref=ref.at[k], dst_ref=ref.at[k], send_sem=kv_send.at[slot, i],
                recv_sem=kv_recv.at[k, i], device_id={"sp": up}, device_id_type=MESH)
            for i, ref in enumerate((kt, vv))
        ]

    def w_copy(k, c, slot, upward):
        mine = g if G == 2 else slice(None)
        source = w.at[mine, :, pl.ds(c * cols, cols)] if slot == 0 else wbuf.at[k, c, mine]
        return pltpu.make_async_remote_copy(
            src_ref=source, dst_ref=wbuf.at[k, c, mine],
            send_sem=(up_send if upward else dn_send).at[slot, c], recv_sem=wz_recv.at[k, c],
            device_id={"sp": up if upward else dn}, device_id_type=MESH)

    def y_copy(k, c, which):
        return pltpu.make_async_remote_copy(
            src_ref=wbuf.at[k, c, which], dst_ref=wbuf.at[k, c, which],
            send_sem=wy_send.at[k, c], recv_sem=wy_recv.at[k, c],
            device_id={"grp": 1 - g}, device_id_type=MESH)

    def st_copy():
        return pltpu.make_async_remote_copy(
            src_ref=st_out, dst_ref=st_in, send_sem=st_send.at[0], recv_sem=st_recv.at[0],
            device_id={"sp": up}, device_id_type=MESH)

    def rs_copy(k, c, o):
        to = lax.rem(j + o, T)
        return pltpu.make_async_remote_copy(
            src_ref=pbuf.at[k, c, to], dst_ref=rbuf.at[o, k, c],
            send_sem=rs_send.at[k, c, o], recv_sem=rs_recv.at[k, c, o],
            device_id={"tp": to}, device_id_type=MESH)

    @pl.when(has_up)
    def _():
        for one in kv_copies(z, 0):
            one.start()
        w_copy(z, 0, 0, True).start()

    @pl.when(has_dn)
    def _():
        for c in range(PARTS):
            w_copy(z, c, 0, False).start()

    inflow = jax.nn.sigmoid(-lb[...]) * jax.nn.sigmoid(-fg[...].astype(F32))
    added = jnp.concatenate(
        [jnp.broadcast_to(ad[h : h + 1, :], (HG_DK, rows)).T for h in range(heads)], axis=1
    )
    logd = jnp.log1p(-inflow) + added
    hi = logd.astype(BF)
    lo = (logd - hi.astype(F32)).astype(BF)
    ti = lax.broadcasted_iota(jnp.int32, (rows, rows), 0)
    si = lax.broadcasted_iota(jnp.int32, (rows, rows), 1)
    tril = ti >= si
    trib = jnp.where(tril, 1.0, 0.0).astype(BF)
    blockb = jnp.where(tril & (ti // CHUNK == si // CHUNK), 1.0, 0.0).astype(BF)
    cum = nn(blockb, hi) + nn(blockb, lo)
    run = nn(trib, hi) + nn(trib, lo)
    q = rq[...].astype(F32)
    qd = (q * jnp.exp(cum)).astype(BF)
    kd = (inflow * jnp.exp(-cum)).astype(BF)
    qrun[...] = (q * jnp.exp(run)).astype(BF)
    total = jnp.exp(run[rows - 1 : rows, :])
    small = (
        lax.broadcasted_iota(jnp.int32, (CHUNK, CHUNK), 0)
        >= lax.broadcasted_iota(jnp.int32, (CHUNK, CHUNK), 1)
    )
    for h in range(heads):
        cs = slice(h * HG_DK, (h + 1) * HG_DK)
        state = None
        for c in range(rows // CHUNK):
            rs = slice(c * CHUNK, (c + 1) * CHUNK)
            vc = rv[rs, cs]
            sc = jnp.where(small, nt(qd[rs, cs], kd[rs, cs]), 0.0).astype(BF)
            o = nn(sc, vc)
            if state is not None:
                o = o + nt(qd[rs, cs], state.astype(BF))
            rec[rs, cs] = o
            last = cum[(c + 1) * CHUNK - 1 : (c + 1) * CHUNK, cs]
            kend = (inflow[rs, cs] * jnp.exp(last - cum[rs, cs])).astype(BF)
            add = tn(vc, kend)
            state = add if state is None else jnp.exp(last) * state + add
        fst[h] = state

    @pl.when(jnp.logical_and(z == 0, has_up))
    def _():
        st_out[...] = fst[...].astype(BF)
        st_copy().start()

    def kv_arrive(d):
        @pl.when(z >= d)
        def _():
            for one in kv_copies(z - d, 0):
                one.wait_recv()

            @pl.when(has_up)
            def _():
                for one in kv_copies(z - d, d):
                    one.start()

    def w_arrive(d, c, upward):
        if d >= S:
            return
        k = z - d if upward else z + d
        there = (z >= d) if upward else (z + d < S)
        onward = has_up if upward else has_dn

        @pl.when(there)
        def _():
            w_copy(k, c, 1, upward).wait_recv()

            @pl.when(onward)
            def _():
                w_copy(k, c, d, upward).start()

            if G == 2:
                y_copy(k, c, g).start()

    q1f = q1[...].astype(F32) * (DA_HD ** -0.5)
    q2f = q2[...].astype(F32) * (DA_HD ** -0.5)
    for h in range(groups):
        a = jnp.concatenate([q1f[:, h * DA_HD : (h + 1) * DA_HD], jnp.zeros((rows, DA_HD), F32)], 1)
        b = jnp.concatenate([jnp.zeros((rows, DA_HD), F32), q2f[:, h * DA_HD : (h + 1) * DA_HD]], 1)
        qs[h] = a.astype(BF)
        qs[groups + h] = b.astype(BF)

    def attend(k, first):
        for r in range(2 * groups):
            s = nn(qs[r], kt[k])
            if first:
                s = jnp.where(tril, s, -1e30)
                top = jnp.max(s, axis=1, keepdims=True)
            else:
                top = jnp.maximum(m_ref[r], jnp.max(s, axis=1, keepdims=True))
            p = jnp.exp(s - top)
            mass = jnp.sum(p, axis=1, keepdims=True)
            val = nn(p.astype(BF), vv[k])
            if not first:
                shrink = jnp.exp(m_ref[r] - top)
                mass = mass + l_ref[r] * shrink
                val = val + acc[r] * shrink
            m_ref[r] = top
            l_ref[r] = mass
            acc[r] = val

    kv_arrive(1)
    w_arrive(1, 0, False)
    attend(z, True)
    if S > 2:
        kv_arrive(2)

    @pl.when(has_dn)
    def _():
        st_copy().wait_recv()

        @pl.when(has_up)
        def _():
            for h in range(heads):
                st_out[h] = (
                    total[:, h * HG_DK : (h + 1) * HG_DK] * st_in[h].astype(F32) + fst[h]
                ).astype(BF)
            st_copy().start()

    @pl.when(has_up)
    def _():
        for c in range(1, PARTS):
            w_copy(z, c, 0, True).start()

    for c in range(1, PARTS):
        w_arrive(1, c, False)
    for d in range(3, S):
        kv_arrive(d)
    for d in range(1, S):
        w_arrive(1 + d, 0, False)

        @pl.when(z >= d)
        def _(d=d):
            attend(z - d, False)

        if d == 1:
            w_arrive(1, 0, True)
        for c in range(1, PARTS):
            w_arrive(1 + d, c, False)

    @pl.when(has_dn)
    def _():
        for h in range(heads):
            cs = slice(h * HG_DK, (h + 1) * HG_DK)
            rec[:, cs] = rec[:, cs] + nt(qrun[:, cs], st_in[h])

    for h in range(heads):
        cs = slice(h * HG_DK, (h + 1) * HG_DK)
        x[:, cs] = head_norm(rec[:, cs], rg[...]).astype(BF)
    for h in range(groups):
        mixed = acc[h] / l_ref[h] - lam[h] * (acc[groups + h] / l_ref[groups + h])
        base = heads * HG_DK + h * 2 * DA_HD
        x[:, base : base + 2 * DA_HD] = head_norm(mixed, ag[...]).astype(BF)

    split = heads * HG_DK

    def project(k, c):
        part = nn(x[:, :split], wbuf[k, c, 0]) + nn(x[:, split:], wbuf[k, c, 1])
        pbuf[k, c] = part.astype(BF).reshape(T, share, cols)
        for o in range(1, T):
            rs_copy(k, c, o).start()

    def finish(d, c, upward):
        k = z - d if upward else z + d

        @pl.when((z >= d) if upward else (z + d < S))
        def _():
            if G == 2:
                y_copy(k, c, 1 - g).wait_recv()
            project(k, c)

    for c in range(1, PARTS):
        w_arrive(1, c, True)
    for c in range(PARTS):
        own_w[c].wait()
        project(z, c)
    for d in range(2, S + 1):
        for c in range(PARTS):
            w_arrive(d, c, True)
        for c in range(PARTS):
            finish(d - 1, c, False)
            finish(d - 1, c, True)

    def gather_piece(k):
        for c in range(PARTS):
            total_sum = pbuf[k, c, j].astype(F32)
            for o in range(1, T):
                rs_copy(k, c, o).wait_recv()
                total_sum = total_sum + rbuf[o, k, c].astype(F32)
            at = pl.multiple_of((k * PARTS + c) * cols, cols)
            out[:, pl.ds(at, cols)] = total_sum.astype(BF)

    gather_piece(z)
    for d in range(1, S):
        for upward in (False, True):
            @pl.when((z >= d) if upward else (z + d < S))
            def _(d=d, upward=upward):
                gather_piece(z - d if upward else z + d)

    @pl.when(has_up)
    def _():
        st_copy().wait_send()

    for d in range(S):
        @pl.when(jnp.logical_and(z >= d, has_up))
        def _(d=d):
            for one in kv_copies(z - d, d):
                one.wait_send()
            for c in range(PARTS):
                w_copy(z - d, c, d, True).wait_send()

        @pl.when(jnp.logical_and(z + d < S, has_dn))
        def _(d=d):
            for c in range(PARTS):
                w_copy(z + d, c, d, False).wait_send()

    for c in range(PARTS):
        if G == 2:
            for d in range(1, S):
                y_copy(lax.rem(z + d, S), c, g).wait_send()
        for k in range(S):
            for o in range(1, T):
                rs_copy(k, c, o).wait_send()


def fused_shards(G, S, T):
    def body(rq, fg, rv, lb, ad, rg, q1, k1, q2, k2, v, lam, ag, w):
        rows, cols = rq.shape[0], w.shape[2] // PARTS
        heads, groups = rq.shape[1] // HG_DK, q1.shape[1] // DA_HD
        vm = pl.BlockSpec(memory_space=pltpu.VMEM)
        specs = [vm] * 14
        specs[11] = pl.BlockSpec(memory_space=pltpu.SMEM)
        specs[13] = pl.BlockSpec(memory_space=pl.ANY)
        dma = pltpu.SemaphoreType.DMA
        return pl.pallas_call(
            lambda *refs: layer_kernel(G, S, T, *refs),
            out_shape=jax.ShapeDtypeStruct((rows // T, w.shape[2] * S), BF),
            in_specs=specs,
            out_specs=vm,
            scratch_shapes=[
                pltpu.VMEM((S, 2 * DA_HD, rows), BF),
                pltpu.VMEM((S, rows, 2 * DA_HD), BF),
                pltpu.VMEM((S, PARTS, 2, w.shape[1], cols), BF),
                pltpu.VMEM((S, PARTS, T, rows // T, cols), BF),
                pltpu.VMEM((T, S, PARTS, rows // T, cols), BF),
                pltpu.VMEM((heads, HG_DV, HG_DK), BF),
                pltpu.VMEM((heads, HG_DV, HG_DK), BF),
                pltpu.VMEM((heads, HG_DV, HG_DK), F32),
                pltpu.VMEM((rows, heads * HG_DV), F32),
                pltpu.VMEM((rows, heads * HG_DK), BF),
                pltpu.VMEM((2 * groups, rows, 2 * DA_HD), BF),
                pltpu.VMEM((2 * groups, rows, 1), F32),
                pltpu.VMEM((2 * groups, rows, 1), F32),
                pltpu.VMEM((2 * groups, rows, 2 * DA_HD), F32),
                pltpu.VMEM((rows, heads * HG_DV + groups * 2 * DA_HD), BF),
                dma((S, 2)), dma((S, 2)), dma((1,)), dma((1,)), dma((S, PARTS)), dma((S, PARTS)),
                dma((S, PARTS)), dma((S, PARTS)), dma((S, PARTS)), dma((S, PARTS, T)),
                dma((S, PARTS, T)), dma((PARTS,)),
            ],
            compiler_params=pltpu.CompilerParams(collective_id=0, has_side_effects=True),
            name="layer",
        )(
            rq, fg, rv, lb.reshape(1, -1), ad.T, rg.reshape(1, -1),
            q1, k1.T, q2, k2.T, v, lam, ag.reshape(1, -1), w,
        )

    return body


def pick(G, S, T):
    def body(*args):
        rows, cols = args[0].shape[0], args[13].shape[2]
        one_key_head = args[7].shape[1] == DA_HD
        if cols % (128 * PARTS) or not one_key_head or S < 2 or G > 2 or rows % (T * 16) or S > 16:
            return shards(*args)
        return fused_shards(G, S, T)(*args)

    return body


def solution(mesh):
    return jax.shard_map(
        pick(mesh.shape["grp"], mesh.shape["sp"], mesh.shape["tp"]),
        mesh=mesh,
        in_specs=(
            P(("grp", "sp"), "tp"),
            P(("grp", "sp"), "tp"),
            P(("grp", "sp"), "tp"),
            P("tp"),
            P(("grp", "sp"), "tp"),
            P(),
            P(("grp", "sp"), "tp"),
            P(("grp", "sp"), "tp"),
            P(("grp", "sp"), "tp"),
            P(("grp", "sp"), "tp"),
            P(("grp", "sp"), "tp"),
            P("tp"),
            P(),
            P(None, "tp", "sp"),
        ),
        out_specs=P(("grp", "sp", "tp"), None),
        check_vma=False,
    )
```
